32 devices in a mesh: sp: 8 (over z, x), tp: 4 (over y, core).
Axes of the slice: x: 2, y: 2, z: 4, core: 2. Of those that a mesh axis runs over, the one named last changes fastest.
Arguments:
- receptance: bfloat16 [2048, 1024], P('sp', 'tp'), may hold values from -6 to 6
- key_vectors: bfloat16 [2048, 1024], P('sp', 'tp'), may hold values from -6 to 6
- values: bfloat16 [2048, 1024], P('sp', 'tp'), may hold values from -6 to 6
- decay_logits: bfloat16 [2048, 1024], P('sp', 'tp'), may hold values from -15 to 1
- correction_logits: bfloat16 [2048, 1024], P('sp', 'tp'), may hold values from -12 to 4
- output_gate: bfloat16 [2048, 1024], P('sp', 'tp'), may hold values from -6 to 6
- extra_log_decay: float32 [2048, 16], P('sp', 'tp'), may hold values from 0 to 0.7
- self_token_weight: float32 [16, 64], P('tp'), may hold values from -1.25 to 1.25
- head_norm_gain: float32 [1024], P('tp'), may hold values from 0.1 to 1.9
- output_weight: bfloat16 [1024, 2048], replicated, may hold values from -0.1875 to 0.1875
- residual_input: bfloat16 [2048, 2048], P(('sp', 'tp')), may hold values from -6 to 6
- expert_norm_gain: float32 [2048], replicated, may hold values from 0.1 to 1.9
- routes: int32 [2048, 4], P('sp'), may hold values from 0 to 7, all different within a row; in each aligned block of 64 rows (0 to 63, 64 to 127, ...) at most 64 rows name the same one
- expert_route_weights: float32 [2048, 4], P(('sp', 'tp')), may hold values from 0.1 to 1
- expert_gate_weight: bfloat16 [8, 2048, 2048], P('sp', None, 'tp'), may hold values from -0.375 to 0.375
- expert_up_weight: bfloat16 [8, 2048, 2048], P('sp', None, 'tp'), may hold values from -0.375 to 0.375
- expert_down_weight: bfloat16 [8, 2048, 2048], P('sp', 'tp'), may hold values from -0.03125 to 0.03125
Outputs:
- layer_out: bfloat16 [2048, 2048], P(('sp', 'tp'))
The draws below stay inside these ranges and needn't reach their ends.
Inputs may be any that keep to these rules, and one draw needn't show every extreme that they name: `routes`: each row names 4 different experts. In each aligned block of 64 rows no expert is named by more than 64 rows, and one is named by exactly 64.
All inputs are finite; a program needn't handle non-finite values.
Results may differ from the reference program's by a relative error of at most 0.019.
Values may be sent and summed in bfloat16 or wider, within the bound.
A program may use at most 128 MiB of HBM per device.

```python
import math
import jax
import jax.numpy as jnp
import numpy as np
from jax import lax

D = 2048
MIXER_HEADS = 16
HEAD_WIDTH = 64
FF = 2048
TOP_K = 4
TOK_DEV = 256
TOKENS = 2048
WIDTH = 1024
EXPERTS = 8
ROWS_DEV = 64
FF_DEV = 512
CAP = 64
N_TP = 4


def slow_heads(key):
    ranking = jax.random.permutation(jax.random.fold_in(key, 101), MIXER_HEADS)
    keep_count = MIXER_HEADS // 2
    return ranking < keep_count


def head_field(key, offset, slow_base, fast_base, shifted):
    slow_mask = slow_heads(key)
    base_level = jnp.where(slow_mask, slow_base, fast_base).astype(jnp.float32)
    jitter = jax.random.truncated_normal(jax.random.fold_in(key, offset), -3.0, 3.0, (TOKENS, MIXER_HEADS, HEAD_WIDTH), jnp.float32)
    levels = base_level[None, :, None] + jitter
    if shifted:
        block_shift = jax.random.uniform(jax.random.fold_in(key, offset + 1), (TOKENS // TOK_DEV, MIXER_HEADS), jnp.float32, -0.7, 0.7)
        levels = levels + jnp.repeat(block_shift, TOK_DEV, axis=0)[:, :, None]
    return levels.reshape(TOKENS, MIXER_HEADS * HEAD_WIDTH).astype(jnp.bfloat16)


def draw_decay_logits(key, part):
    return head_field(key, 202, -11.0, -3.5, True)


def draw_correction_logits(key, part):
    return head_field(key, 303, -8.0, 0.0, False)


def draw_extra_log_decay(key, part):
    third = TOKENS // 3
    offsets = jax.random.randint(jax.random.fold_in(key, 404), (3, MIXER_HEADS), 0, third)
    positions = offsets + (jnp.arange(3, dtype=jnp.int32) * third)[:, None]
    depths = jax.random.uniform(jax.random.fold_in(key, 405), (3, MIXER_HEADS), jnp.float32, 0.22, 0.69)
    places = jnp.arange(TOKENS, dtype=jnp.int32)[:, None, None]
    return jnp.sum(jnp.where(places == positions[None], depths[None], 0.0), axis=1)


def steps_of(key, shape, cuts, smallest, top_value):
    gain = 1.0
    for position, parts in cuts:
        steps = jax.random.uniform(jax.random.fold_in(jax.random.fold_in(key, 6), position), (parts,), jnp.float32, smallest / len(cuts), top_value / len(cuts))
        gain = gain * jnp.repeat(jnp.exp(steps), shape[position] // parts).reshape((-1,) + (1,) * (len(shape) - 1 - position))
    return gain


def assign_block(rng, own, number, rows, amount, top, most, lean):
    sequence = jax.random.permutation(rng, amount)
    packed, usual = shares(amount, rows * top, most, lean, True), shares(amount, rows * top, most, lean, False)
    places = jnp.arange(amount)

    def named(sizes, rotation):
        used = int((sizes > 0).sum())
        fixed = max(1, used // 4)
        moved = fixed + (places - fixed + rotation * (used - fixed)) % max(1, amount - fixed)
        return jnp.zeros((amount,), jnp.int32).at[sequence[jnp.where(places < fixed, places, moved)]].set(jnp.asarray(sizes, jnp.int32))

    sizes = jnp.where(number % 4 == 0, named(packed, number // 4), named(usual, number - number // 4 - 1))
    mixed = jax.random.permutation(jax.random.fold_in(own, 3), amount)
    giver, sink = mixed[0:amount // 2 * 2:2], mixed[1:amount // 2 * 2:2]
    room = jnp.minimum(sizes[giver] - 1, most - sizes[sink]) // 2
    room = jnp.where((giver == sequence[0]) | (sink == sequence[0]) | (sizes[sink] == 0), 0, jnp.maximum(room, 0))
    moved = jax.random.randint(jax.random.fold_in(own, 4), (amount // 2,), 0, 1 << 20) % (room + 1)
    sizes = sizes.at[giver].add(-moved).at[sink].add(moved)
    members = jnp.searchsorted(jnp.cumsum(sizes), jnp.arange(rows * top), side="right").astype(jnp.int32)
    table = members.reshape(top, rows).T
    table = table[jax.random.permutation(jax.random.fold_in(own, 1), rows)]
    rotation = jax.random.randint(jax.random.fold_in(own, 2), (rows, 1), 0, top)
    return jnp.take_along_axis(table, (jnp.arange(top)[None, :] + rotation) % top, axis=1)


def shares(amount, total, most, lean, full):
    weights = [(1 << 20) // math.isqrt(rank ** lean) + 1 for rank in range(1, amount + 1)]
    largest = most if full else min(most, max(-(-total // amount), total * weights[0] // sum(weights)))
    least = 1 if total - largest >= amount - 1 else 0
    given, surplus = [largest] + [least] * (amount - 1), total - largest - least * (amount - 1)
    while surplus > 0:
        candidates = [i for i in range(1, amount) if given[i] < largest] or [i for i in range(1, amount) if given[i] < most]
        pool, budget = sum([weights[i] for i in candidates]), surplus
        for i in candidates:
            addition = min(most - given[i], max(1, budget * weights[i] // pool), surplus)
            given[i] = given[i] + addition
            surplus = surplus - addition
    return np.array(given)


def centred(key, dims, width, limit, pieces=(), held_as=jnp.bfloat16):
    drawn = jax.random.normal(key, dims, jnp.float32) * width
    if len(pieces) > 0:
        drawn = steps_of(key, dims, pieces, -0.22, 0.18) * drawn
    return jnp.clip(drawn, min=-limit, max=limit).astype(held_as)


def setup_inputs(seed: int = 0) -> dict:
    key_of = jax.random.split(jax.random.key(seed), 18)
    receptance = centred(key_of[0], (TOKENS, WIDTH), 1.0, 6.0, ((0, 8), (1, 4)))
    key_vectors = centred(key_of[1], (TOKENS, WIDTH), 1.0, 6.0, ((0, 8), (1, 4)))
    values = centred(key_of[2], (TOKENS, WIDTH), 1.0, 6.0, ((0, 8), (1, 4)))
    decay_logits = draw_decay_logits(jax.random.fold_in(key_of[17], 71), 0)
    correction_logits = draw_correction_logits(jax.random.fold_in(key_of[17], 71), 0)
    output_gate = centred(key_of[5], (TOKENS, WIDTH), 1.0, 6.0, ((0, 8), (1, 4)))
    extra_log_decay = draw_extra_log_decay(jax.random.fold_in(key_of[17], 71), 0)
    self_token_weight = centred(key_of[7], (MIXER_HEADS, HEAD_WIDTH), 0.2, 1.25, ((0, 4),), jnp.float32)
    head_norm_gain = jnp.clip(1.0 + 0.18 * jax.random.normal(key_of[8], (WIDTH,), jnp.float32), 0.1, 1.9)
    output_weight = centred(key_of[9], (WIDTH, D), WIDTH ** -0.5, 0.1875)
    residual_input = centred(key_of[10], (TOKENS, D), 1.0, 6.0, ((0, 32),))
    expert_norm_gain = jnp.clip(1.0 + 0.18 * jax.random.normal(key_of[11], (D,), jnp.float32), 0.1, 1.9)
    routes_keys = jax.random.split(jax.random.fold_in(key_of[12], 1), TOKENS // ROWS_DEV)
    routes_turns = jax.random.permutation(jax.random.fold_in(key_of[12], 3), TOKENS // ROWS_DEV)
    routes = jax.vmap(lambda own, number: assign_block(jax.random.fold_in(key_of[12], 2), own, number, ROWS_DEV, EXPERTS, TOP_K, CAP, 2))(routes_keys, routes_turns).reshape((TOKENS, TOP_K))
    expert_route_weights = jnp.clip(0.1 + 0.9 * jax.random.uniform(key_of[13], (TOKENS, TOP_K), jnp.float32) ** steps_of(key_of[13], (TOKENS, TOP_K), ((0, 32),), -0.2, 0.2), 0.1, 1.0)
    expert_gate_weight = centred(key_of[14], (EXPERTS, D, FF), (D // 9) ** -0.5, 0.375, ((0, 8), (2, 4)))
    expert_up_weight = centred(key_of[15], (EXPERTS, D, FF), (D // 9) ** -0.5, 0.375, ((0, 8), (2, 4)))
    expert_down_weight = centred(key_of[16], (EXPERTS, FF, D), (16 * FF) ** -0.5, 0.03125, ((0, 8), (1, 4)))
    return dict(receptance=receptance, key_vectors=key_vectors, values=values, decay_logits=decay_logits, correction_logits=correction_logits, output_gate=output_gate, extra_log_decay=extra_log_decay, self_token_weight=self_token_weight, head_norm_gain=head_norm_gain, output_weight=output_weight, residual_input=residual_input, expert_norm_gain=expert_norm_gain, routes=routes, expert_route_weights=expert_route_weights, expert_gate_weight=expert_gate_weight, expert_up_weight=expert_up_weight, expert_down_weight=expert_down_weight)


group_eps = 0.00064
norm_eps = 1e-06
clamp_limit = 7.0
swish_alpha = 1.702
row_block = 256
highest = lax.Precision.HIGHEST

def mixer_input_rows(receptance, key_vectors, values, decay_logits, correction_logits, extra_log_decay, token_count, number_heads, head_width):
    reshaped_rows = (token_count, number_heads, head_width)
    readout_query = receptance.astype(jnp.float32).reshape(reshaped_rows)
    key_product = key_vectors.astype(jnp.float32).reshape(reshaped_rows)
    value_product = values.astype(jnp.float32).reshape(reshaped_rows)
    rate_logarithm = -jax.nn.softplus(-decay_logits.astype(jnp.float32)) - 0.5
    decay_logarithm = (-jnp.exp(rate_logarithm)).reshape(reshaped_rows) - extra_log_decay[:, :, None]
    removal = jax.nn.sigmoid(correction_logits.astype(jnp.float32)).reshape(reshaped_rows)
    normalized_keys = key_product * lax.rsqrt(lax.optimization_barrier(jnp.sum(key_product * key_product, axis=-1, keepdims=True)) + norm_eps)
    return (readout_query, key_product, value_product, decay_logarithm, normalized_keys, normalized_keys * removal)

def complete_heads(readout_rows, readout_query, key_product, value_product, output_gate, self_token_weight, head_norm_gain):
    number_heads, head_width = self_token_weight.shape
    centre = lax.optimization_barrier(jnp.mean(readout_rows, axis=-1, keepdims=True))
    spread_sq = lax.optimization_barrier(jnp.mean(jnp.square(readout_rows - centre), axis=-1, keepdims=True))
    normalized_rows = (readout_rows - centre) * lax.rsqrt(spread_sq + group_eps) * head_norm_gain.reshape(number_heads, head_width)
    self_token_term = lax.optimization_barrier(jnp.sum(readout_query * key_product * self_token_weight, axis=-1, keepdims=True)) * value_product
    mixer_rows = (normalized_rows + self_token_term).reshape(readout_rows.shape[0], number_heads * head_width) * output_gate.astype(jnp.float32)
    return mixer_rows.astype(jnp.bfloat16)

def rms_rows(stream, expert_norm_gain):
    widened = stream.astype(jnp.float32)
    scaled = widened * lax.rsqrt(lax.optimization_barrier(jnp.mean(widened * widened, axis=-1, keepdims=True)) + norm_eps) * expert_norm_gain
    return scaled.astype(jnp.bfloat16)

def expert_act(block_rows, gate_matrix, up_matrix):
    gate_pre = jnp.dot(block_rows, gate_matrix, preferred_element_type=jnp.float32)
    up_pre = jnp.dot(block_rows, up_matrix, preferred_element_type=jnp.float32)
    gated = jnp.minimum(gate_pre, clamp_limit)
    lifted = jnp.clip(up_pre, -clamp_limit, clamp_limit) + 1.0
    return (lifted * gated * jax.nn.sigmoid(swish_alpha * gated)).astype(jnp.bfloat16)

def reference(receptance, key_vectors, values, decay_logits, correction_logits, output_gate, extra_log_decay, self_token_weight, head_norm_gain, output_weight, residual_input, expert_norm_gain, routes, expert_route_weights, expert_gate_weight, expert_up_weight, expert_down_weight):
    number_heads, head_width = self_token_weight.shape
    token_count = receptance.shape[0]
    readout_query, key_product, value_product, decay_logarithm, normalized_keys, correction_amount = mixer_input_rows(receptance, key_vectors, values, decay_logits, correction_logits, extra_log_decay, token_count, number_heads, head_width)

    def advance(carried, inputs):
        decay_t, unit_t, removed_t, value_t, key_t, read_t = inputs
        projected = jnp.einsum('hvk,hk->hv', carried, unit_t, precision=highest)
        carried = carried * decay_t[:, None, :] - projected[:, :, None] * removed_t[:, None, :] + value_t[:, :, None] * key_t[:, None, :]
        return (carried, jnp.einsum('hvk,hk->hv', carried, read_t, precision=highest))
    initial = jnp.zeros((number_heads, head_width, head_width), jnp.float32)
    _, readout_rows = lax.scan(advance, initial, (jnp.exp(decay_logarithm), normalized_keys, correction_amount, value_product, key_product, readout_query))
    mixer_rows = complete_heads(readout_rows, readout_query, key_product, value_product, output_gate, self_token_weight, head_norm_gain)
    mixer_out = jnp.dot(mixer_rows, output_weight, preferred_element_type=jnp.float32)
    stream = (residual_input.astype(jnp.float32) + mixer_out).astype(jnp.bfloat16)
    normed_rows = rms_rows(stream, expert_norm_gain)
    model_width = stream.shape[1]
    assign_count = token_count * TOP_K
    flattened = routes.reshape(-1).astype(jnp.int32)
    ordering = jnp.argsort(flattened, stable=True).astype(jnp.int32)
    expert_ids = jnp.arange(EXPERTS, dtype=jnp.int32)
    per_expert = lax.optimization_barrier(jnp.sum((flattened[:, None] == expert_ids[None, :]).astype(jnp.int32), axis=0))
    rounded_up = (per_expert + row_block - 1) // row_block * row_block
    block_ends = jnp.cumsum(rounded_up).astype(jnp.int32)
    block_starts = block_ends - rounded_up
    sorted_starts = (jnp.cumsum(per_expert) - per_expert).astype(jnp.int32)
    sorted_ids = flattened[ordering]
    destination = block_starts[sorted_ids] + jnp.arange(assign_count, dtype=jnp.int32) - sorted_starts[sorted_ids]
    block_total = (assign_count + EXPERTS * (row_block - 1)) // row_block
    row_source = jnp.full((block_total * row_block,), assign_count, jnp.int32).at[destination].set(ordering)
    block_index = jnp.arange(block_total, dtype=jnp.int32)[:, None] * row_block
    block_expert = jnp.minimum(lax.optimization_barrier(jnp.sum((block_ends[None, :] <= block_index).astype(jnp.int32), axis=1)), EXPERTS - 1).astype(jnp.int32)
    padded_rows = jnp.concatenate([normed_rows, jnp.zeros((1, model_width), jnp.bfloat16)], axis=0)
    padded_weights = jnp.concatenate([expert_route_weights.reshape(-1), jnp.zeros((1,), jnp.float32)])

    def expert_block(collected, inputs):
        expert, sources = inputs
        token_ids = sources // TOP_K
        block_rows = padded_rows[token_ids]
        activated = expert_act(block_rows, expert_gate_weight[expert], expert_up_weight[expert])
        down_rows = expert_down_weight[expert]
        summed = jnp.zeros((row_block, model_width), jnp.float32)
        for group_index in range(N_TP):
            lower = group_index * FF_DEV
            partial_value = jnp.dot(activated[:, lower:lower + FF_DEV], down_rows[lower:lower + FF_DEV], preferred_element_type=jnp.float32).astype(jnp.bfloat16)
            partial_value = lax.optimization_barrier(partial_value)
            summed = summed + partial_value.astype(jnp.float32)
        expert_rows = summed.astype(jnp.bfloat16)
        weighted = padded_weights[sources][:, None] * expert_rows.astype(jnp.float32)
        return (collected.at[token_ids].add(weighted), None)
    collected = jnp.zeros((token_count + 1, model_width), jnp.float32)
    collected, _ = lax.scan(expert_block, collected, (block_expert, row_source.reshape(block_total, row_block)))
    return (stream.astype(jnp.float32) + collected[:token_count]).astype(jnp.bfloat16)
```

```python
import functools
import math

import jax
import jax.numpy as jnp
from jax import lax
from jax.experimental import pallas as pl
from jax.experimental.pallas import tpu as pltpu
from jax.sharding import PartitionSpec as P

group_eps = 0.00064
norm_eps = 1e-06
clamp_limit = 7.0
swish_alpha = 1.702
HI = lax.Precision.HIGHEST


def nn(a, b):
    return lax.dot_general(a, b, (((1,), (0,)), ((), ())), precision=HI, preferred_element_type=jnp.float32)


def nt(a, b):
    return lax.dot_general(a, b, (((1,), (1,)), ((), ())), precision=HI, preferred_element_type=jnp.float32)


def tn(a, b):
    return lax.dot_general(a, b, (((0,), (0,)), ((), ())), precision=HI, preferred_element_type=jnp.float32)


def iota2(shape, axis):
    return lax.broadcasted_iota(jnp.int32, shape, axis)


def sigmoid(x):
    return 1.0 / (1.0 + jnp.exp(-x))


def head_ones(width, head_width):
    same = iota2((width, width), 0) // head_width == iota2((width, width), 1) // head_width
    return same.astype(jnp.float32)


def mixer_kernel(heads, length, r_ref, k_ref, v_ref, dl_ref, cl_ref, ex_ref, q_ref, r0_ref, gh_ref, ms_ref):
    tokens, width = r_ref.shape
    hw = width // heads
    chunks = tokens // length
    r = r_ref[...].astype(jnp.float32)
    k = k_ref[...].astype(jnp.float32)
    v = v_ref[...].astype(jnp.float32)
    ex = jnp.concatenate(
        [jnp.broadcast_to(ex_ref[:, h : h + 1], (tokens, hw)) for h in range(heads)], axis=1
    )
    logd = -math.exp(-0.5) * sigmoid(dl_ref[...].astype(jnp.float32)) - ex
    u = k * lax.rsqrt(nn(k * k, head_ones(width, hw)) + norm_eps)
    c = u * sigmoid(cl_ref[...].astype(jnp.float32))
    row, col = iota2((length, length), 0), iota2((length, length), 1)
    inclusive = (col <= row).astype(jnp.float32)
    strict = (col < row).astype(jnp.float32)
    eye = (col == row).astype(jnp.float32)
    levels = []
    size = 1
    while size < length:
        levels.append(
            ((row // (2 * size) == col // (2 * size)) & (row // size != col // size) & (col < row)).astype(
                jnp.float32
            )
        )
        size *= 2
    totals = [None] * heads
    for i in range(chunks):
        rows = slice(i * length, (i + 1) * length)
        kc, vc, uc, cc, rc = k[rows], v[rows], u[rows], c[rows], r[rows]
        run = nn(inclusive, logd[rows])
        before = run - logd[rows]
        mid = run[length // 2 : length // 2 + 1]
        last = run[length - 1 : length]
        fall = jnp.exp(mid - run)
        tail = jnp.exp(last - run)
        rising = jnp.concatenate([uc * jnp.exp(before - mid), rc * jnp.exp(run - mid)], axis=0)
        falling = jnp.concatenate([cc * fall, kc * fall], axis=0)
        ub, rb = uc * jnp.exp(before), rc * jnp.exp(run)
        kt, ct = kc * tail, cc * tail
        decay = jnp.exp(last)
        for h in range(heads):
            ch = slice(h * hw, (h + 1) * hw)
            pair = nt(rising[:, ch], falling[:, ch])
            low = pair[:length, :length] * strict
            k2u = pair[:length, length:] * strict
            c2r = pair[length:, :length] * inclusive
            k2r = pair[length:, length:] * inclusive
            inv = eye - low * levels[0]
            for mask in levels[1:]:
                inv = inv - nn(nn(inv, low * mask), inv)
            vh = vc[:, ch]
            w = nn(inv, ub[:, ch])
            y = nn(inv, nn(k2u, vh))
            q_ref[rows, ch] = rb[:, ch] - nn(c2r, w)
            r0_ref[rows, ch] = nn(k2r, vh) - nn(c2r, y)
            g = jnp.where(iota2((hw, hw), 0) == iota2((hw, hw), 1), decay[:, ch], 0.0) - tn(w, ct[:, ch])
            s = tn(vh, kt[:, ch]) - tn(y, ct[:, ch])
            gh_ref[i, h, :, :hw] = g
            gh_ref[i, h, :, hw:] = s
            if i == 0:
                totals[h] = (g, s)
            else:
                totals[h] = (nn(totals[h][0], g), nn(totals[h][1], g) + s)
    for h in range(heads):
        ms_ref[h, :, :hw] = totals[h][0].astype(jnp.bfloat16)
        ms_ref[h, :, hw:] = totals[h][1].astype(jnp.bfloat16)


def chain_kernel(
    n, heads, length, ms_ref, q_ref, r0_ref, gh_ref, r_ref, k_ref, v_ref, gate_ref, stw_ref, gain_ref,
    out_ref, buf, prior, reads, send_sem, recv_sem,
):
    tokens, width = q_ref.shape
    hw = width // heads
    me = lax.axis_index("sp")
    barrier = pltpu.get_barrier_semaphore()
    for d in range(1, n):
        pl.semaphore_signal(
            barrier, inc=1, device_id={"sp": lax.rem(me + d, n)}, device_id_type=pl.DeviceIdType.MESH
        )
    pl.semaphore_wait(barrier, n - 1)

    def copy(d):
        return pltpu.make_async_remote_copy(
            src_ref=ms_ref,
            dst_ref=buf.at[d - 1],
            send_sem=send_sem.at[d - 1],
            recv_sem=recv_sem.at[d - 1],
            device_id={"sp": lax.rem(me + d, n)},
            device_id_type=pl.DeviceIdType.MESH,
        )

    for d in range(1, n):
        copy(d).start()
    ones = head_ones(width, hw)
    r = r_ref[...].astype(jnp.float32)
    k = k_ref[...].astype(jnp.float32)
    v = v_ref[...].astype(jnp.float32)
    self_term = nn(r * k * stw_ref[...], ones) * v
    for d in range(1, n):
        copy(d).wait()
    prior[...] = jnp.zeros_like(prior)

    def compose(j, carry):
        slot = me - j - 1
        for h in range(heads):
            block = buf[slot, h].astype(jnp.float32)
            prior[h] = nn(prior[h], block[:, :hw]) + block[:, hw:]
        return carry

    lax.fori_loop(0, me, compose, 0)
    states = [prior[h] for h in range(heads)]
    for i in range(tokens // length):
        rows = slice(i * length, (i + 1) * length)
        for h in range(heads):
            ch = slice(h * hw, (h + 1) * hw)
            reads[rows, ch] = r0_ref[rows, ch] + nt(q_ref[rows, ch], states[h])
            states[h] = nn(states[h], gh_ref[i, h, :, :hw]) + gh_ref[i, h, :, hw:]
    read = reads[...]
    centred = read - nn(read, ones) * (1.0 / hw)
    spread = nn(centred * centred, ones) * (1.0 / hw)
    mixed = centred * lax.rsqrt(spread + group_eps) * gain_ref[...] + self_term
    out_ref[...] = (mixed * gate_ref[...].astype(jnp.float32)).astype(jnp.bfloat16)


def vmem(count):
    return [pl.BlockSpec(memory_space=pltpu.VMEM)] * count


def mixer(r, k, v, dl, cl, gate, extra, self_token_weight, head_norm_gain):
    tokens, width = r.shape
    heads, hw = self_token_weight.shape
    n = lax.axis_size("sp")
    length = min(64, tokens)
    chunks = tokens // length
    f32 = jnp.float32
    q, r0, gh, ms = pl.pallas_call(
        functools.partial(mixer_kernel, heads, length),
        out_shape=(
            jax.ShapeDtypeStruct((tokens, width), f32),
            jax.ShapeDtypeStruct((tokens, width), f32),
            jax.ShapeDtypeStruct((chunks, heads, hw, 2 * hw), f32),
            jax.ShapeDtypeStruct((heads, hw, 2 * hw), jnp.bfloat16),
        ),
        in_specs=vmem(6),
        out_specs=tuple(vmem(4)),
        cost_estimate=pl.CostEstimate(flops=10**10, bytes_accessed=10**7, transcendentals=10**6),
    )(r, k, v, dl, cl, extra)
    return pl.pallas_call(
        functools.partial(chain_kernel, n, heads, length),
        out_shape=jax.ShapeDtypeStruct((tokens, width), jnp.bfloat16),
        in_specs=vmem(10),
        out_specs=pl.BlockSpec(memory_space=pltpu.VMEM),
        scratch_shapes=[
            pltpu.VMEM((n - 1, heads, hw, 2 * hw), jnp.bfloat16),
            pltpu.VMEM((heads, hw, hw), f32),
            pltpu.VMEM((tokens, width), f32),
            pltpu.SemaphoreType.DMA((n - 1,)),
            pltpu.SemaphoreType.DMA((n - 1,)),
        ],
        compiler_params=pltpu.CompilerParams(collective_id=0, has_side_effects=True),
        cost_estimate=pl.CostEstimate(flops=10**10, bytes_accessed=10**7, transcendentals=10**6),
    )(ms, q, r0, gh, r, k, v, gate, self_token_weight.reshape(1, width), head_norm_gain.reshape(1, width))


def layer_kernel(parts, mix_ref, res_ref, ow_ref, gain_ref, wt_ref, gw_ref, uw_ref, dw_ref, part_ref, stream_ref):
    width = mix_ref.shape[3]
    acc = res_ref[...].astype(jnp.float32)
    for t in range(parts):
        acc += jnp.dot(
            mix_ref[0, t], ow_ref[t * width : (t + 1) * width], preferred_element_type=jnp.float32
        )
    stream = acc.astype(jnp.bfloat16)
    stream_ref[...] = stream
    wide = stream.astype(jnp.float32)
    normed = (
        wide * lax.rsqrt(jnp.mean(wide * wide, axis=-1, keepdims=True) + norm_eps) * gain_ref[...]
    ).astype(jnp.bfloat16)
    act = expert_act(normed, gw_ref[0], uw_ref[0])
    part = jnp.dot(act, dw_ref[0], preferred_element_type=jnp.float32)
    part_ref[...] = (part * wt_ref[...]).astype(jnp.bfloat16)


def dense_layer(
    mixer_rows, residual_input, output_weight, expert_norm_gain, routes, route_weights, gw, uw, dw
):
    n, parts = lax.axis_size("sp"), lax.axis_size("tp")
    row_count, model_width = residual_input.shape
    own = lax.dynamic_slice_in_dim(routes, lax.axis_index("tp") * row_count, row_count, 0)
    experts = jnp.arange(n, dtype=jnp.int32)
    table = jnp.sum(
        jnp.where(own[:, :, None] == experts, route_weights[:, :, None], 0.0), axis=1
    )
    high = lax.reduce_precision(table, 8, 7)
    middle = lax.reduce_precision(table - high, 8, 7)
    extra = jnp.concatenate([high, middle, table - high - middle], axis=1).astype(jnp.bfloat16)
    extra = jnp.pad(extra, ((0, 0), (0, -extra.shape[1] % 128)))
    early = lax.all_gather(
        jnp.concatenate([residual_input, extra], axis=1), ("sp", "tp"), axis=0, tiled=True
    )
    side = lax.dynamic_slice_in_dim(early, model_width, extra.shape[1], 1).astype(jnp.float32)
    place = lax.axis_index("sp")
    weight = sum(
        lax.dynamic_slice_in_dim(side, place + j * n, 1, 1) for j in range(3)
    )
    tokens, width = mixer_rows.shape
    mixed = lax.all_gather(mixer_rows, ("sp", "tp"), axis=0).reshape(n, parts, tokens, width)
    ff = gw.shape[2]
    total = n * tokens

    def whole(*shape):
        return pl.BlockSpec(shape, lambda i: (0,) * len(shape), pipeline_mode=pl.Buffered(1))

    part, stream = pl.pallas_call(
        functools.partial(layer_kernel, parts),
        grid=(n,),
        out_shape=(
            jax.ShapeDtypeStruct((total, model_width), jnp.bfloat16),
            jax.ShapeDtypeStruct((total, model_width), jnp.bfloat16),
        ),
        in_specs=[
            pl.BlockSpec((1, parts, tokens, width), lambda i: (i, 0, 0, 0)),
            pl.BlockSpec((tokens, model_width), lambda i: (i, 0)),
            whole(parts * width, model_width),
            whole(1, model_width),
            pl.BlockSpec((tokens, 1), lambda i: (i, 0)),
            whole(1, model_width, ff),
            whole(1, model_width, ff),
            whole(1, ff, model_width),
        ],
        out_specs=(
            pl.BlockSpec((tokens, model_width), lambda i: (i, 0)),
            pl.BlockSpec((tokens, model_width), lambda i: (i, 0)),
        ),
        compiler_params=pltpu.CompilerParams(vmem_limit_bytes=60 * 2**20),
    )(mixed, early, output_weight, expert_norm_gain.reshape(1, -1), weight, gw, uw, dw)
    summed = lax.psum_scatter(part, ("sp", "tp"), scatter_dimension=0, tiled=True)
    place = lax.axis_index(("sp", "tp")) * row_count
    own_stream = lax.dynamic_slice_in_dim(stream, place, row_count, 0)
    return (own_stream.astype(jnp.float32) + summed.astype(jnp.float32)).astype(jnp.bfloat16)


def rms_rows(stream, expert_norm_gain):
    widened = stream.astype(jnp.float32)
    scaled = (
        widened
        * lax.rsqrt(jnp.mean(widened * widened, axis=-1, keepdims=True) + norm_eps)
        * expert_norm_gain
    )
    return scaled.astype(jnp.bfloat16)


def expert_act(block_rows, gate_matrix, up_matrix):
    gate_pre = jnp.dot(block_rows, gate_matrix, preferred_element_type=jnp.float32)
    up_pre = jnp.dot(block_rows, up_matrix, preferred_element_type=jnp.float32)
    gated = jnp.minimum(gate_pre, clamp_limit)
    lifted = jnp.clip(up_pre, -clamp_limit, clamp_limit) + 1.0
    return (lifted * gated * sigmoid(swish_alpha * gated)).astype(jnp.bfloat16)


def slot_plan(route_rows, limit, expert_total):
    flattened = route_rows.reshape(-1)
    assign_count = flattened.shape[0]
    onehot = (flattened[:, None] == jnp.arange(expert_total, dtype=jnp.int32)[None, :]).astype(
        jnp.int32
    )
    earlier_count = jnp.cumsum(onehot, axis=0) - onehot
    position = jnp.sum(earlier_count * onehot, axis=1)
    slot_ids = flattened * limit + position
    source_table = (
        jnp.full((expert_total * limit,), assign_count, jnp.int32)
        .at[slot_ids]
        .set(jnp.arange(assign_count, dtype=jnp.int32))
    )
    return (slot_ids, source_table)


def shards(
    receptance,
    key_vectors,
    values,
    decay_logits,
    correction_logits,
    output_gate,
    extra_log_decay,
    self_token_weight,
    head_norm_gain,
    output_weight,
    residual_input,
    expert_norm_gain,
    routes,
    expert_route_weights,
    expert_gate_weight,
    expert_up_weight,
    expert_down_weight,
):
    mixer_rows = mixer(
        receptance,
        key_vectors,
        values,
        decay_logits,
        correction_logits,
        output_gate,
        extra_log_decay,
        self_token_weight,
        head_norm_gain,
    )
    row_count, top_count = expert_route_weights.shape
    expert_total = lax.axis_size("sp")
    capacity = max(2, 2 * row_count * top_count // expert_total)
    if capacity >= row_count:
        return dense_layer(
            mixer_rows,
            residual_input,
            output_weight,
            expert_norm_gain,
            routes,
            expert_route_weights,
            expert_gate_weight,
            expert_up_weight,
            expert_down_weight,
        )
    by_token = lax.all_to_all(mixer_rows, "tp", split_axis=0, concat_axis=1, tiled=True)
    mixer_out = jnp.dot(by_token, output_weight, preferred_element_type=jnp.float32)
    stream = (residual_input.astype(jnp.float32) + mixer_out).astype(jnp.bfloat16)
    normed_rows = rms_rows(stream, expert_norm_gain)
    model_width = stream.shape[1]
    zero_row = jnp.zeros((1, model_width), jnp.bfloat16)
    own_routes = lax.dynamic_slice_in_dim(routes, lax.axis_index("tp") * row_count, row_count, 0)
    slot_ids, source_table = slot_plan(own_routes, capacity, expert_total)
    padded_own = jnp.concatenate([normed_rows, zero_row], axis=0)
    outgoing = padded_own[source_table // top_count].reshape(expert_total, capacity, model_width)
    arrived = lax.all_to_all(outgoing, "sp", split_axis=0, concat_axis=0, tiled=True)
    flattened = arrived.reshape(-1, model_width)
    activated = expert_act(
        lax.all_gather(flattened, "tp", axis=0, tiled=True),
        expert_gate_weight[0],
        expert_up_weight[0],
    )
    partial_value = jnp.dot(
        activated, expert_down_weight[0], preferred_element_type=jnp.float32
    ).astype(jnp.bfloat16)
    summed = lax.psum_scatter(
        lax.optimization_barrier(partial_value).astype(jnp.float32).astype(jnp.bfloat16),
        "tp",
        scatter_dimension=0,
        tiled=True,
    )
    returned = lax.all_to_all(
        summed.reshape(arrived.shape), "sp", split_axis=0, concat_axis=0, tiled=True
    )
    expert_rows = returned.reshape(-1, model_width)[slot_ids].reshape(
        row_count, top_count, model_width
    )
    weighted = jnp.sum(expert_route_weights[:, :, None] * expert_rows.astype(jnp.float32), axis=1)
    return (stream.astype(jnp.float32) + weighted).astype(jnp.bfloat16)


def solution(mesh):
    in_specs = (
        P("sp", "tp"),
        P("sp", "tp"),
        P("sp", "tp"),
        P("sp", "tp"),
        P("sp", "tp"),
        P("sp", "tp"),
        P("sp", "tp"),
        P("tp", None),
        P("tp"),
        P(),
        P(("sp", "tp"), None),
        P(),
        P("sp", None),
        P(("sp", "tp"), None),
        P("sp", None, "tp"),
        P("sp", None, "tp"),
        P("sp", "tp", None),
    )
    out_specs = P(("sp", "tp"), None)
    return jax.shard_map(shards, mesh=mesh, in_specs=in_specs, out_specs=out_specs, check_vma=False)
```

```python
import functools
import math

import jax
import jax.numpy as jnp
from jax import lax
from jax.experimental import pallas as pl
from jax.experimental.pallas import tpu as pltpu
from jax.sharding import PartitionSpec as P

group_eps = 0.00064
norm_eps = 1e-06
clamp_limit = 7.0
swish_alpha = 1.702
HI = lax.Precision.HIGHEST


def nn(a, b):
    return lax.dot_general(a, b, (((1,), (0,)), ((), ())), precision=HI, preferred_element_type=jnp.float32)


def nt(a, b):
    return lax.dot_general(a, b, (((1,), (1,)), ((), ())), precision=HI, preferred_element_type=jnp.float32)


def tn(a, b):
    return lax.dot_general(a, b, (((0,), (0,)), ((), ())), precision=HI, preferred_element_type=jnp.float32)


def iota2(shape, axis):
    return lax.broadcasted_iota(jnp.int32, shape, axis)


def sigmoid(x):
    return 1.0 / (1.0 + jnp.exp(-x))


def head_ones(width, head_width):
    same = iota2((width, width), 0) // head_width == iota2((width, width), 1) // head_width
    return same.astype(jnp.float32)


def mixer_kernel(heads, length, r_ref, k_ref, v_ref, dl_ref, cl_ref, ex_ref, q_ref, r0_ref, gh_ref, ms_ref):
    tokens, width = r_ref.shape
    hw = width // heads
    chunks = tokens // length
    r = r_ref[...].astype(jnp.float32)
    k = k_ref[...].astype(jnp.float32)
    v = v_ref[...].astype(jnp.float32)
    ex = jnp.concatenate(
        [jnp.broadcast_to(ex_ref[:, h : h + 1], (tokens, hw)) for h in range(heads)], axis=1
    )
    logd = -math.exp(-0.5) * sigmoid(dl_ref[...].astype(jnp.float32)) - ex
    u = k * lax.rsqrt(nn(k * k, head_ones(width, hw)) + norm_eps)
    c = u * sigmoid(cl_ref[...].astype(jnp.float32))
    row, col = iota2((length, length), 0), iota2((length, length), 1)
    inclusive = (col <= row).astype(jnp.float32)
    strict = (col < row).astype(jnp.float32)
    eye = (col == row).astype(jnp.float32)
    levels = []
    size = 1
    while size < length:
        levels.append(
            ((row // (2 * size) == col // (2 * size)) & (row // size != col // size) & (col < row)).astype(
                jnp.float32
            )
        )
        size *= 2
    totals = [None] * heads
    for i in range(chunks):
        rows = slice(i * length, (i + 1) * length)
        kc, vc, uc, cc, rc = k[rows], v[rows], u[rows], c[rows], r[rows]
        run = nn(inclusive, logd[rows])
        before = run - logd[rows]
        mid = run[length // 2 : length // 2 + 1]
        last = run[length - 1 : length]
        fall = jnp.exp(mid - run)
        tail = jnp.exp(last - run)
        rising = jnp.concatenate([uc * jnp.exp(before - mid), rc * jnp.exp(run - mid)], axis=0)
        falling = jnp.concatenate([cc * fall, kc * fall], axis=0)
        ub, rb = uc * jnp.exp(before), rc * jnp.exp(run)
        kt, ct = kc * tail, cc * tail
        decay = jnp.exp(last)
        for h in range(heads):
            ch = slice(h * hw, (h + 1) * hw)
            pair = nt(rising[:, ch], falling[:, ch])
            low = pair[:length, :length] * strict
            k2u = pair[:length, length:] * strict
            c2r = pair[length:, :length] * inclusive
            k2r = pair[length:, length:] * inclusive
            inv = eye - low * levels[0]
            for mask in levels[1:]:
                inv = inv - nn(nn(inv, low * mask), inv)
            vh = vc[:, ch]
            w = nn(inv, ub[:, ch])
            y = nn(inv, nn(k2u, vh))
            q_ref[rows, ch] = rb[:, ch] - nn(c2r, w)
            r0_ref[rows, ch] = nn(k2r, vh) - nn(c2r, y)
            g = jnp.where(iota2((hw, hw), 0) == iota2((hw, hw), 1), decay[:, ch], 0.0) - tn(w, ct[:, ch])
            s = tn(vh, kt[:, ch]) - tn(y, ct[:, ch])
            gh_ref[i, h, :, :hw] = g
            gh_ref[i, h, :, hw:] = s
            if i == 0:
                totals[h] = (g, s)
            else:
                totals[h] = (nn(totals[h][0], g), nn(totals[h][1], g) + s)
    for h in range(heads):
        ms_ref[h, :, :hw] = totals[h][0].astype(jnp.bfloat16)
        ms_ref[h, :, hw:] = totals[h][1].astype(jnp.bfloat16)


def chain_kernel(
    n, heads, length, ms_ref, q_ref, r0_ref, gh_ref, r_ref, k_ref, v_ref, gate_ref, stw_ref, gain_ref,
    out_ref, buf, prior, reads, send_sem, recv_sem,
):
    tokens, width = q_ref.shape
    hw = width // heads
    me = lax.axis_index("sp")
    barrier = pltpu.get_barrier_semaphore()
    for d in range(1, n):
        pl.semaphore_signal(
            barrier, inc=1, device_id={"sp": lax.rem(me + d, n)}, device_id_type=pl.DeviceIdType.MESH
        )
    pl.semaphore_wait(barrier, n - 1)

    def copy(d):
        return pltpu.make_async_remote_copy(
            src_ref=ms_ref,
            dst_ref=buf.at[d - 1],
            send_sem=send_sem.at[d - 1],
            recv_sem=recv_sem.at[d - 1],
            device_id={"sp": lax.rem(me + d, n)},
            device_id_type=pl.DeviceIdType.MESH,
        )

    for d in range(1, n):
        copy(d).start()
    ones = head_ones(width, hw)
    r = r_ref[...].astype(jnp.float32)
    k = k_ref[...].astype(jnp.float32)
    v = v_ref[...].astype(jnp.float32)
    self_term = nn(r * k * stw_ref[...], ones) * v
    for d in range(1, n):
        copy(d).wait()
    prior[...] = jnp.zeros_like(prior)

    def compose(j, carry):
        slot = me - j - 1
        for h in range(heads):
            block = buf[slot, h].astype(jnp.float32)
            prior[h] = nn(prior[h], block[:, :hw]) + block[:, hw:]
        return carry

    lax.fori_loop(0, me, compose, 0)
    states = [prior[h] for h in range(heads)]
    for i in range(tokens // length):
        rows = slice(i * length, (i + 1) * length)
        for h in range(heads):
            ch = slice(h * hw, (h + 1) * hw)
            reads[rows, ch] = r0_ref[rows, ch] + nt(q_ref[rows, ch], states[h])
            states[h] = nn(states[h], gh_ref[i, h, :, :hw]) + gh_ref[i, h, :, hw:]
    read = reads[...]
    centred = read - nn(read, ones) * (1.0 / hw)
    spread = nn(centred * centred, ones) * (1.0 / hw)
    mixed = centred * lax.rsqrt(spread + group_eps) * gain_ref[...] + self_term
    out_ref[...] = (mixed * gate_ref[...].astype(jnp.float32)).astype(jnp.bfloat16)


def vmem(count):
    return [pl.BlockSpec(memory_space=pltpu.VMEM)] * count


def mixer(r, k, v, dl, cl, gate, extra, self_token_weight, head_norm_gain):
    tokens, width = r.shape
    heads, hw = self_token_weight.shape
    n = lax.axis_size("sp")
    length = min(64, tokens)
    chunks = tokens // length
    f32 = jnp.float32
    q, r0, gh, ms = pl.pallas_call(
        functools.partial(mixer_kernel, heads, length),
        out_shape=(
            jax.ShapeDtypeStruct((tokens, width), f32),
            jax.ShapeDtypeStruct((tokens, width), f32),
            jax.ShapeDtypeStruct((chunks, heads, hw, 2 * hw), f32),
            jax.ShapeDtypeStruct((heads, hw, 2 * hw), jnp.bfloat16),
        ),
        in_specs=vmem(6),
        out_specs=tuple(vmem(4)),
        cost_estimate=pl.CostEstimate(flops=10**10, bytes_accessed=10**7, transcendentals=10**6),
    )(r, k, v, dl, cl, extra)
    return pl.pallas_call(
        functools.partial(chain_kernel, n, heads, length),
        out_shape=jax.ShapeDtypeStruct((tokens, width), jnp.bfloat16),
        in_specs=vmem(10),
        out_specs=pl.BlockSpec(memory_space=pltpu.VMEM),
        scratch_shapes=[
            pltpu.VMEM((n - 1, heads, hw, 2 * hw), jnp.bfloat16),
            pltpu.VMEM((heads, hw, hw), f32),
            pltpu.VMEM((tokens, width), f32),
            pltpu.SemaphoreType.DMA((n - 1,)),
            pltpu.SemaphoreType.DMA((n - 1,)),
        ],
        compiler_params=pltpu.CompilerParams(collective_id=0, has_side_effects=True),
        cost_estimate=pl.CostEstimate(flops=10**10, bytes_accessed=10**7, transcendentals=10**6),
    )(ms, q, r0, gh, r, k, v, gate, self_token_weight.reshape(1, width), head_norm_gain.reshape(1, width))


def layer_kernel(parts, mix_ref, res_ref, ow_ref, gain_ref, wt_ref, gw_ref, uw_ref, dw_ref, part_ref, stream_ref):
    width = mix_ref.shape[3]
    acc = res_ref[...].astype(jnp.float32)
    for t in range(parts):
        acc += jnp.dot(
            mix_ref[0, t], ow_ref[t * width : (t + 1) * width], preferred_element_type=jnp.float32
        )
    stream = acc.astype(jnp.bfloat16)
    stream_ref[...] = stream
    wide = stream.astype(jnp.float32)
    normed = (
        wide * lax.rsqrt(jnp.mean(wide * wide, axis=-1, keepdims=True) + norm_eps) * gain_ref[...]
    ).astype(jnp.bfloat16)
    act = expert_act(normed, gw_ref[0], uw_ref[0])
    part = jnp.dot(act, dw_ref[0], preferred_element_type=jnp.float32)
    part_ref[...] = (part * wt_ref[...]).astype(jnp.bfloat16).reshape(part_ref.shape)


def dense_layer(
    mixer_rows, residual_input, output_weight, expert_norm_gain, routes, route_weights, gw, uw, dw
):
    n, parts = lax.axis_size("sp"), lax.axis_size("tp")
    row_count, model_width = residual_input.shape
    own = lax.dynamic_slice_in_dim(routes, lax.axis_index("tp") * row_count, row_count, 0)
    experts = jnp.arange(n, dtype=jnp.int32)
    table = jnp.sum(
        jnp.where(own[:, :, None] == experts, route_weights[:, :, None], 0.0), axis=1
    )
    high = lax.reduce_precision(table, 8, 7)
    middle = lax.reduce_precision(table - high, 8, 7)
    extra = jnp.concatenate([high, middle, table - high - middle], axis=1).astype(jnp.bfloat16)
    extra = jnp.pad(extra, ((0, 0), (0, -extra.shape[1] % 128)))
    early = lax.all_gather(
        jnp.concatenate([residual_input, extra], axis=1), ("sp", "tp"), axis=0, tiled=True
    )
    side = lax.dynamic_slice_in_dim(early, model_width, extra.shape[1], 1).astype(jnp.float32)
    place = lax.axis_index("sp")
    weight = sum(
        lax.dynamic_slice_in_dim(side, place + j * n, 1, 1) for j in range(3)
    )
    tokens, width = mixer_rows.shape
    mixed = lax.all_gather(mixer_rows, ("sp", "tp"), axis=0).reshape(n, parts, tokens, width)
    ff = gw.shape[2]
    total = n * tokens

    def whole(*shape):
        return pl.BlockSpec(shape, lambda i: (0,) * len(shape), pipeline_mode=pl.Buffered(1))

    part, stream = pl.pallas_call(
        functools.partial(layer_kernel, parts),
        grid=(n,),
        out_shape=(
            jax.ShapeDtypeStruct((parts, n, row_count, model_width), jnp.bfloat16),
            jax.ShapeDtypeStruct((total, model_width), jnp.bfloat16),
        ),
        in_specs=[
            pl.BlockSpec((1, parts, tokens, width), lambda i: (i, 0, 0, 0)),
            pl.BlockSpec((tokens, model_width), lambda i: (i, 0)),
            whole(parts * width, model_width),
            whole(1, model_width),
            pl.BlockSpec((tokens, 1), lambda i: (i, 0)),
            whole(1, model_width, ff),
            whole(1, model_width, ff),
            whole(1, ff, model_width),
        ],
        out_specs=(
            pl.BlockSpec((parts, 1, row_count, model_width), lambda i: (0, i, 0, 0)),
            pl.BlockSpec((tokens, model_width), lambda i: (i, 0)),
        ),
        compiler_params=pltpu.CompilerParams(vmem_limit_bytes=60 * 2**20),
    )(mixed, early, output_weight, expert_norm_gain.reshape(1, -1), weight, gw, uw, dw)
    part = part.reshape(total, model_width)
    summed = lax.psum_scatter(part, "tp", scatter_dimension=0, tiled=True)
    summed = lax.psum_scatter(summed, "sp", scatter_dimension=0, tiled=True)
    place = lax.axis_index(("sp", "tp")) * row_count
    own_stream = lax.dynamic_slice_in_dim(stream, place, row_count, 0)
    return (own_stream.astype(jnp.float32) + summed.astype(jnp.float32)).astype(jnp.bfloat16)


def rms_rows(stream, expert_norm_gain):
    widened = stream.astype(jnp.float32)
    scaled = (
        widened
        * lax.rsqrt(jnp.mean(widened * widened, axis=-1, keepdims=True) + norm_eps)
        * expert_norm_gain
    )
    return scaled.astype(jnp.bfloat16)


def expert_act(block_rows, gate_matrix, up_matrix):
    gate_pre = jnp.dot(block_rows, gate_matrix, preferred_element_type=jnp.float32)
    up_pre = jnp.dot(block_rows, up_matrix, preferred_element_type=jnp.float32)
    gated = jnp.minimum(gate_pre, clamp_limit)
    lifted = jnp.clip(up_pre, -clamp_limit, clamp_limit) + 1.0
    return (lifted * gated * sigmoid(swish_alpha * gated)).astype(jnp.bfloat16)


def slot_plan(route_rows, limit, expert_total):
    flattened = route_rows.reshape(-1)
    assign_count = flattened.shape[0]
    onehot = (flattened[:, None] == jnp.arange(expert_total, dtype=jnp.int32)[None, :]).astype(
        jnp.int32
    )
    earlier_count = jnp.cumsum(onehot, axis=0) - onehot
    position = jnp.sum(earlier_count * onehot, axis=1)
    slot_ids = flattened * limit + position
    source_table = (
        jnp.full((expert_total * limit,), assign_count, jnp.int32)
        .at[slot_ids]
        .set(jnp.arange(assign_count, dtype=jnp.int32))
    )
    return (slot_ids, source_table)


def shards(
    receptance,
    key_vectors,
    values,
    decay_logits,
    correction_logits,
    output_gate,
    extra_log_decay,
    self_token_weight,
    head_norm_gain,
    output_weight,
    residual_input,
    expert_norm_gain,
    routes,
    expert_route_weights,
    expert_gate_weight,
    expert_up_weight,
    expert_down_weight,
):
    mixer_rows = mixer(
        receptance,
        key_vectors,
        values,
        decay_logits,
        correction_logits,
        output_gate,
        extra_log_decay,
        self_token_weight,
        head_norm_gain,
    )
    row_count, top_count = expert_route_weights.shape
    expert_total = lax.axis_size("sp")
    capacity = max(2, 2 * row_count * top_count // expert_total)
    if capacity >= row_count:
        return dense_layer(
            mixer_rows,
            residual_input,
            output_weight,
            expert_norm_gain,
            routes,
            expert_route_weights,
            expert_gate_weight,
            expert_up_weight,
            expert_down_weight,
        )
    by_token = lax.all_to_all(mixer_rows, "tp", split_axis=0, concat_axis=1, tiled=True)
    mixer_out = jnp.dot(by_token, output_weight, preferred_element_type=jnp.float32)
    stream = (residual_input.astype(jnp.float32) + mixer_out).astype(jnp.bfloat16)
    normed_rows = rms_rows(stream, expert_norm_gain)
    model_width = stream.shape[1]
    zero_row = jnp.zeros((1, model_width), jnp.bfloat16)
    own_routes = lax.dynamic_slice_in_dim(routes, lax.axis_index("tp") * row_count, row_count, 0)
    slot_ids, source_table = slot_plan(own_routes, capacity, expert_total)
    padded_own = jnp.concatenate([normed_rows, zero_row], axis=0)
    outgoing = padded_own[source_table // top_count].reshape(expert_total, capacity, model_width)
    arrived = lax.all_to_all(outgoing, "sp", split_axis=0, concat_axis=0, tiled=True)
    flattened = arrived.reshape(-1, model_width)
    activated = expert_act(
        lax.all_gather(flattened, "tp", axis=0, tiled=True),
        expert_gate_weight[0],
        expert_up_weight[0],
    )
    partial_value = jnp.dot(
        activated, expert_down_weight[0], preferred_element_type=jnp.float32
    ).astype(jnp.bfloat16)
    summed = lax.psum_scatter(
        lax.optimization_barrier(partial_value).astype(jnp.float32).astype(jnp.bfloat16),
        "tp",
        scatter_dimension=0,
        tiled=True,
    )
    returned = lax.all_to_all(
        summed.reshape(arrived.shape), "sp", split_axis=0, concat_axis=0, tiled=True
    )
    expert_rows = returned.reshape(-1, model_width)[slot_ids].reshape(
        row_count, top_count, model_width
    )
    weighted = jnp.sum(expert_route_weights[:, :, None] * expert_rows.astype(jnp.float32), axis=1)
    return (stream.astype(jnp.float32) + weighted).astype(jnp.bfloat16)


def solution(mesh):
    in_specs = (
        P("sp", "tp"),
        P("sp", "tp"),
        P("sp", "tp"),
        P("sp", "tp"),
        P("sp", "tp"),
        P("sp", "tp"),
        P("sp", "tp"),
        P("tp", None),
        P("tp"),
        P(),
        P(("sp", "tp"), None),
        P(),
        P("sp", None),
        P(("sp", "tp"), None),
        P("sp", None, "tp"),
        P("sp", None, "tp"),
        P("sp", "tp", None),
    )
    out_specs = P(("sp", "tp"), None)
    return jax.shard_map(shards, mesh=mesh, in_specs=in_specs, out_specs=out_specs, check_vma=False)
```
